32 devices in a mesh: grp: 2 (over y), fs: 4 (over z), tp: 4 (over x, core).
Axes of the slice: x: 2, y: 2, z: 4, core: 2. Of those that a mesh axis runs over, the one named last changes fastest.
Arguments:
- tokens: bfloat16 [3072, 2048], P(('grp', 'fs'), 'tp'), parts along dimension 0, may hold values from -25 to 25
- gain_first: float32 [2048], replicated, may hold values from 0.1 to 1.9
- gate_first: bfloat16 [2048, 5120], P('fs', 'tp'), may hold values from -0.125 to 0.125
- up_first: bfloat16 [2048, 5120], P('fs', 'tp'), may hold values from -0.125 to 0.125
- down_first: bfloat16 [5120, 2048], P('tp', 'fs'), may hold values from -0.078125 to 0.078125
- gain_mixer: float32 [2048], replicated, may hold values from 0.1 to 1.9
- outer_gate: bfloat16 [2048, 1024], P('fs', 'tp'), may hold values from -0.125 to 0.125
- inner_gate: bfloat16 [2048, 1024], P('fs', 'tp'), may hold values from -0.125 to 0.125
- conv_input: bfloat16 [2048, 1024], P('fs', 'tp'), may hold values from -0.125 to 0.125
- conv_taps: float32 [3, 1024], P(None, 'tp'), may hold values from -3.5 to 3.5
- mixer_out: bfloat16 [1024, 2048], P('tp', 'fs'), may hold values from -0.1875 to 0.1875
- gain_last: float32 [2048], replicated, may hold values from 0.1 to 1.9
- gate_last: bfloat16 [2048, 5120], P('fs', 'tp'), may hold values from -0.125 to 0.125
- up_last: bfloat16 [2048, 5120], P('fs', 'tp'), may hold values from -0.125 to 0.125
- down_last: bfloat16 [5120, 2048], P('tp', 'fs'), may hold values from -0.078125 to 0.078125
Outputs:
- layer_out: bfloat16 [3072, 2048], P(('grp', 'fs'), 'tp'), parts along dimension 0
The draws below stay inside these ranges and needn't reach their ends.
There are 2 independent parts, one for each index of `grp`. The reference program is written for one: setup_inputs(seed, part) draws one part's arguments, and reference() takes and returns one part's arrays. A program takes and returns all parts, laid end to end along the dimension named above; an argument that names none is the same for every part. Nothing has to cross between parts.
All inputs are finite; a program needn't handle non-finite values.
Results may differ from the reference program's by a relative error of at most 0.015.
Values may be sent and summed in bfloat16 or wider, within the bound.
A program may use at most 64 MiB of HBM per device.

```python
import math
import jax
import jax.numpy as jnp
from jax import lax

D = 2048
FF = 5120
SC = 1024
KERNEL = 3
SEQ_LEN = 64
TOKENS = 1536
N_TP = 4


def draw_tokens(key, part):
    row_count = TOKENS
    col_count = D
    key_base, key_row, key_col = jax.random.split(jax.random.fold_in(key, 11), 3)
    values_raw = jnp.clip(jax.random.normal(key_base, (row_count, col_count), jnp.float32), -4.0, 4.0)
    row_scale = jnp.exp(jax.random.uniform(key_row, (row_count, 1), jnp.float32, math.log(0.5), math.log(2.0)))
    rising = 0.5 * jnp.power(4.0, jnp.arange(col_count, dtype=jnp.float32) / col_count)
    jitter = jnp.exp(jax.random.uniform(key_col, (col_count,), jnp.float32, -0.4, 0.4))
    return (values_raw * row_scale * (rising * jitter)[None, :]).astype(jnp.bfloat16)


def block_levels(key, shape, cuts, smallest, top_value):
    loudness = 1.0
    for position, shards_of in cuts:
        draws = jax.random.uniform(jax.random.fold_in(jax.random.fold_in(key, 6), position), (shards_of,), jnp.float32, smallest / len(cuts), top_value / len(cuts))
        loudness = loudness * jnp.repeat(jnp.exp(draws), shape[position] // shards_of).reshape((-1,) + (1,) * (len(shape) - 1 - position))
    return loudness


def scatter_about(key, shape, spread, limit, pieces=(), kind=jnp.bfloat16):
    drawn = spread * jax.random.normal(key, shape, jnp.float32)
    if pieces:
        drawn = drawn * block_levels(key, shape, pieces, -0.22, 0.18)
    return jnp.clip(drawn, -limit, limit).astype(kind)


def setup_inputs(seed: int = 0, part: int = 0) -> dict:
    key_of = jax.random.split(jax.random.key(seed), 16)
    part_keys = jax.random.split(jax.random.fold_in(key_of[15], part), 16)
    tokens = draw_tokens(jax.random.fold_in(jax.random.fold_in(key_of[15], part), 71), part)
    gain_first = jnp.clip(1.0 + 0.18 * jax.random.normal(key_of[1], (D,), jnp.float32), 0.1, 1.9)
    gate_first = scatter_about(key_of[2], (D, FF), D ** -0.5, 0.125, ((0, 4), (1, 4)))
    up_first = scatter_about(key_of[3], (D, FF), D ** -0.5, 0.125, ((0, 4), (1, 4)))
    down_first = scatter_about(key_of[4], (FF, D), FF ** -0.5, 0.078125, ((0, 4), (1, 4)))
    gain_mixer = jnp.clip(1.0 + 0.18 * jax.random.normal(key_of[5], (D,), jnp.float32), 0.1, 1.9)
    outer_gate = scatter_about(key_of[6], (D, SC), D ** -0.5, 0.125, ((0, 4), (1, 4)))
    inner_gate = scatter_about(key_of[7], (D, SC), D ** -0.5, 0.125, ((0, 4), (1, 4)))
    conv_input = scatter_about(key_of[8], (D, SC), D ** -0.5, 0.125, ((0, 4), (1, 4)))
    conv_taps = scatter_about(key_of[9], (KERNEL, SC), KERNEL ** -0.5, 3.5, ((1, 4),), jnp.float32)
    mixer_out = scatter_about(key_of[10], (SC, D), SC ** -0.5, 0.1875, ((0, 4), (1, 4)))
    gain_last = jnp.clip(1.0 + 0.18 * jax.random.normal(key_of[11], (D,), jnp.float32), 0.1, 1.9)
    gate_last = scatter_about(key_of[12], (D, FF), D ** -0.5, 0.125, ((0, 4), (1, 4)))
    up_last = scatter_about(key_of[13], (D, FF), D ** -0.5, 0.125, ((0, 4), (1, 4)))
    down_last = scatter_about(key_of[14], (FF, D), FF ** -0.5, 0.078125, ((0, 4), (1, 4)))
    return dict(tokens=tokens, gain_first=gain_first, gate_first=gate_first, up_first=up_first, down_first=down_first, gain_mixer=gain_mixer, outer_gate=outer_gate, inner_gate=inner_gate, conv_input=conv_input, conv_taps=conv_taps, mixer_out=mixer_out, gain_last=gain_last, gate_last=gate_last, up_last=up_last, down_last=down_last)


norm_eps = 1e-06

def rms_rows(residual, gain_vec):
    inverse = lax.rsqrt(lax.optimization_barrier(jnp.mean(residual * residual, axis=1, keepdims=True)) + norm_eps)
    return (residual * inverse * gain_vec).astype(jnp.bfloat16)

def blocked_sum(left_rows, right_rows):
    extent = left_rows.shape[1] // N_TP
    running = jnp.zeros((left_rows.shape[0], right_rows.shape[1]), jnp.float32)
    for block_id in range(N_TP):
        branch = jnp.dot(left_rows[:, block_id * extent:(block_id + 1) * extent], right_rows[block_id * extent:(block_id + 1) * extent], preferred_element_type=jnp.float32).astype(jnp.bfloat16)
        running = running + lax.optimization_barrier(branch).astype(jnp.float32)
    return running

def causal_mixing(gated, conv_taps):
    row_count, channels = gated.shape
    shaped = gated.reshape(row_count // SEQ_LEN, SEQ_LEN, channels)
    kernel = conv_taps.shape[0]
    padded = jnp.pad(shaped, ((0, 0), (kernel - 1, 0), (0, 0)))
    result = jnp.zeros_like(shaped)
    for offset in range(kernel):
        result = result + conv_taps[offset] * padded[:, offset:offset + SEQ_LEN]
    return result.reshape(row_count, channels)

def half_step(residual, gain_vec, gate_weight, up_weight, down_weight):
    normed = rms_rows(residual, gain_vec)
    gate_pre = jnp.dot(normed, gate_weight, preferred_element_type=jnp.float32)
    up_pre = jnp.dot(normed, up_weight, preferred_element_type=jnp.float32)
    hidden = (jax.nn.silu(gate_pre) * up_pre).astype(jnp.bfloat16)
    return residual + 0.5 * blocked_sum(hidden, down_weight)

def reference(tokens, gain_first, gate_first, up_first, down_first, gain_mixer, outer_gate, inner_gate, conv_input, conv_taps, mixer_out, gain_last, gate_last, up_last, down_last):
    residual = tokens.astype(jnp.float32)
    residual = half_step(residual, gain_first, gate_first, up_first, down_first)
    normed = rms_rows(residual, gain_mixer)
    outer_pre = jnp.dot(normed, outer_gate, preferred_element_type=jnp.float32)
    inner_pre = jnp.dot(normed, inner_gate, preferred_element_type=jnp.float32)
    value_pre = jnp.dot(normed, conv_input, preferred_element_type=jnp.float32)
    convolved = causal_mixing(inner_pre * value_pre, conv_taps)
    mixed_rows = (outer_pre * convolved).astype(jnp.bfloat16)
    residual = residual + blocked_sum(mixed_rows, mixer_out)
    residual = half_step(residual, gain_last, gate_last, up_last, down_last)
    return residual.astype(jnp.bfloat16)
```

```python
import jax
import jax.numpy as jnp
from jax import lax
from jax.sharding import PartitionSpec as P

SEQ_LEN = 64


norm_eps = 1e-06


def scaled_rows(residual, gain_vec, inverse):
    return (residual * inverse * gain_vec).astype(jnp.bfloat16)


def causal_mixing(gated, conv_taps):
    row_count, channels = gated.shape
    shaped = gated.reshape(row_count // SEQ_LEN, SEQ_LEN, channels)
    kernel = conv_taps.shape[0]
    padded = jnp.pad(shaped, ((0, 0), (kernel - 1, 0), (0, 0)))
    result = jnp.zeros_like(shaped)
    for offset in range(kernel):
        result = result + conv_taps[offset] * padded[:, offset : offset + SEQ_LEN]
    return result.reshape(row_count, channels)


def make_shards(groups, ring, parts):
    def shift(value, axis, size, by):
        return lax.ppermute(value, axis, [(i, (i + by) % size) for i in range(size)])

    def shards(
        tokens,
        gain_first,
        gate_first,
        up_first,
        down_first,
        gain_mixer,
        outer_gate,
        inner_gate,
        conv_input,
        conv_taps,
        mixer_out,
        gain_last,
        gate_last,
        up_last,
        down_last,
    ):
        column_count = tokens.shape[1]
        width = column_count * parts
        grain = width // (ring * groups)
        g = lax.axis_index("grp")
        z = lax.axis_index("fs")
        t = lax.axis_index("tp")

        def gather(weight, axis):
            pieces = [
                lax.dynamic_slice_in_dim(weight, (g + j) % groups * grain, grain, axis)
                for j in range(groups)
            ]
            travelling = pieces[0]
            for _ in range(1, ring):
                travelling = shift(travelling, "fs", ring, 1)
                pieces.append(travelling)
                for j in range(1, groups):
                    pieces.append(shift(travelling, "grp", groups, -j))
            return pieces

        def arrival_order(value):
            axis = value.ndim - 1
            blocks = []
            for r in range(ring):
                for j in range(groups):
                    start = ((z - r) % ring * groups + (g + j) % groups) * grain
                    blocks.append(lax.dynamic_slice_in_dim(value, start, grain, axis))
            return jnp.concatenate(blocks, axis)

        def own_columns(value, owner):
            blocks = []
            for k in range(column_count // grain):
                block = owner * (column_count // grain) + k
                shard, half = block // groups, block % groups
                place = (z - shard) % ring * groups + (half - g) % groups
                blocks.append(lax.dynamic_slice_in_dim(value, place * grain, grain, 1))
            return jnp.concatenate(blocks, 1)

        gate_first, up_first = gather(gate_first, 0), gather(up_first, 0)
        down_first = gather(down_first, 1)
        entries = gather(jnp.concatenate((outer_gate, inner_gate, conv_input), 1), 0)
        mixer_out = gather(mixer_out, 1)
        gate_last, up_last = gather(gate_last, 0), gather(up_last, 0)
        down_last = gather(down_last, 1)

        def into(normed, pieces):
            return jnp.dot(
                normed, jnp.concatenate(pieces, 0), preferred_element_type=jnp.float32
            )

        def out_of(hidden, pieces):
            return jnp.concatenate(
                [
                    jnp.dot(hidden, piece, preferred_element_type=jnp.float32).astype(
                        jnp.bfloat16
                    )
                    for piece in pieces
                ],
                1,
            )

        def normalize(residual, gain_vec):
            inverse = lax.rsqrt(jnp.mean(residual * residual, axis=1, keepdims=True) + norm_eps)
            return scaled_rows(residual, gain_vec, inverse)

        def hidden_units(normed, gate_pieces, up_pieces):
            gate_pre, up_pre = into(normed, gate_pieces), into(normed, up_pieces)
            return (jax.nn.silu(gate_pre) * up_pre).astype(jnp.bfloat16)

        def add_branch(residual, branch, factor):
            return residual + factor * lax.psum(branch, "tp").astype(jnp.float32)

        residual = arrival_order(lax.all_gather(tokens, "tp", axis=1, tiled=True))
        residual = residual.astype(jnp.float32)

        normed = normalize(residual, arrival_order(gain_first))
        hidden = hidden_units(normed, gate_first, up_first)
        residual = add_branch(residual, out_of(hidden, down_first), 0.5)

        normed = normalize(residual, arrival_order(gain_mixer))
        channels = entries[0].shape[1] // 3
        projected = into(normed, entries)
        outer_pre, inner_pre, value_pre = (
            projected[:, i * channels : (i + 1) * channels] for i in range(3)
        )
        convolved = causal_mixing(inner_pre * value_pre, conv_taps)
        mixed_rows = (outer_pre * convolved).astype(jnp.bfloat16)
        residual = add_branch(residual, out_of(mixed_rows, mixer_out), 1.0)

        normed = normalize(residual, arrival_order(gain_last))
        hidden = hidden_units(normed, gate_last, up_last)
        branch = out_of(hidden, down_last)
        total = own_columns(branch, t).astype(jnp.float32)
        for k in range(1, parts):
            theirs = own_columns(branch, (t + k) % parts)
            total = total + shift(theirs, "tp", parts, k).astype(jnp.float32)
        return (own_columns(residual, t) + 0.5 * total).astype(jnp.bfloat16)

    return shards


def solution(mesh):
    in_specs = (
        P(("grp", "fs"), "tp"),
        P(),
        P("fs", "tp"),
        P("fs", "tp"),
        P("tp", "fs"),
        P(),
        P("fs", "tp"),
        P("fs", "tp"),
        P("fs", "tp"),
        P(None, "tp"),
        P("tp", "fs"),
        P(),
        P("fs", "tp"),
        P("fs", "tp"),
        P("tp", "fs"),
    )
    out_specs = P(("grp", "fs"), "tp")
    shards = make_shards(mesh.shape["grp"], mesh.shape["fs"], mesh.shape["tp"])
    return jax.shard_map(shards, mesh=mesh, in_specs=in_specs, out_specs=out_specs, check_vma=False)
```

```python
import jax
import jax.numpy as jnp
from jax import lax
from jax.sharding import PartitionSpec as P

SEQ_LEN = 64


norm_eps = 1e-06


def scaled_rows(residual, gain_vec, inverse):
    return (residual * inverse * gain_vec).astype(jnp.bfloat16)


def causal_mixing(gated, conv_taps):
    row_count, channels = gated.shape
    shaped = gated.reshape(row_count // SEQ_LEN, SEQ_LEN, channels)
    kernel = conv_taps.shape[0]
    padded = jnp.pad(shaped, ((0, 0), (kernel - 1, 0), (0, 0)))
    result = jnp.zeros_like(shaped)
    for offset in range(kernel):
        result = result + conv_taps[offset] * padded[:, offset : offset + SEQ_LEN]
    return result.reshape(row_count, channels)


def make_shards(groups, ring, parts):
    def shift(value, axis, size, by):
        return lax.ppermute(value, axis, [(i, (i + by) % size) for i in range(size)])

    def shards(
        tokens,
        gain_first,
        gate_first,
        up_first,
        down_first,
        gain_mixer,
        outer_gate,
        inner_gate,
        conv_input,
        conv_taps,
        mixer_out,
        gain_last,
        gate_last,
        up_last,
        down_last,
    ):
        column_count = tokens.shape[1]
        width = column_count * parts
        grain = width // (ring * groups)
        g = lax.axis_index("grp")
        z = lax.axis_index("fs")
        t = lax.axis_index("tp")

        def gather(batches, flights):
            pieces = {}
            landed = []
            for batch in batches:
                for name, (weight, axis) in batch.items():
                    pieces[name] = [weight]
                travelling = {
                    name: lax.dynamic_slice_in_dim(weight, g * grain, grain, axis)
                    for name, (weight, axis) in batch.items()
                }
                for _ in range(1, ring):
                    for name in batch:
                        block = travelling[name]
                        if len(landed) >= flights:
                            block, _ = lax.optimization_barrier((block, landed[-flights]))
                        block = shift(block, "fs", ring, 1)
                        landed.append(block)
                        travelling[name] = block
                        pieces[name].append(block)
                        for j in range(1, groups):
                            pieces[name].append(shift(block, "grp", groups, -j))
            return pieces

        def arrival_order(value):
            axis = value.ndim - 1
            blocks = [lax.dynamic_slice_in_dim(value, z * groups * grain, groups * grain, axis)]
            for r in range(1, ring):
                for j in range(groups):
                    start = ((z - r) % ring * groups + (g + j) % groups) * grain
                    blocks.append(lax.dynamic_slice_in_dim(value, start, grain, axis))
            return jnp.concatenate(blocks, axis)

        def own_columns(value, owner):
            blocks = []
            for k in range(column_count // grain):
                block = owner * (column_count // grain) + k
                shard, half = block // groups, block % groups
                turn = (z - shard) % ring
                place = turn * groups + jnp.where(turn == 0, half, (half - g) % groups)
                blocks.append(lax.dynamic_slice_in_dim(value, place * grain, grain, 1))
            return jnp.concatenate(blocks, 1)

        pieces = gather(
            (
                {"gate_first": (gate_first, 0), "up_first": (up_first, 0), "down_first": (down_first, 1)},
                {
                    "entries": (jnp.concatenate((outer_gate, inner_gate, conv_input), 1), 0),
                    "mixer_out": (mixer_out, 1),
                },
                {"gate_last": (gate_last, 0), "up_last": (up_last, 0), "down_last": (down_last, 1)},
            ),
            4,
        )

        def into(normed, pieces):
            total, start = 0.0, 0
            for piece in pieces:
                rows = normed[:, start : start + piece.shape[0]]
                total = total + jnp.dot(rows, piece, preferred_element_type=jnp.float32)
                start += piece.shape[0]
            return total

        def out_of(hidden, pieces):
            return jnp.concatenate(
                [
                    jnp.dot(hidden, piece, preferred_element_type=jnp.float32).astype(
                        jnp.bfloat16
                    )
                    for piece in pieces
                ],
                1,
            )

        def normalize(residual, gain_vec):
            inverse = lax.rsqrt(jnp.mean(residual * residual, axis=1, keepdims=True) + norm_eps)
            return scaled_rows(residual, gain_vec, inverse)

        def hidden_units(normed, gate_pieces, up_pieces):
            gate_pre, up_pre = into(normed, gate_pieces), into(normed, up_pieces)
            return (jax.nn.silu(gate_pre) * up_pre).astype(jnp.bfloat16)

        def add_branch(residual, branch, factor):
            return residual + factor * lax.psum(branch, "tp").astype(jnp.float32)

        residual = arrival_order(lax.all_gather(tokens, "tp", axis=1, tiled=True))
        residual = residual.astype(jnp.float32)

        normed = normalize(residual, arrival_order(gain_first))
        hidden = hidden_units(normed, pieces["gate_first"], pieces["up_first"])
        residual = add_branch(residual, out_of(hidden, pieces["down_first"]), 0.5)

        normed = normalize(residual, arrival_order(gain_mixer))
        channels = pieces["entries"][0].shape[1] // 3
        projected = into(normed, pieces["entries"])
        outer_pre, inner_pre, value_pre = (
            projected[:, i * channels : (i + 1) * channels] for i in range(3)
        )
        convolved = causal_mixing(inner_pre * value_pre, conv_taps)
        mixed_rows = (outer_pre * convolved).astype(jnp.bfloat16)
        residual = add_branch(residual, out_of(mixed_rows, pieces["mixer_out"]), 1.0)

        normed = normalize(residual, arrival_order(gain_last))
        hidden = hidden_units(normed, pieces["gate_last"], pieces["up_last"])
        branch = out_of(hidden, pieces["down_last"])
        total = own_columns(branch, t).astype(jnp.float32)
        for k in range(1, parts):
            theirs = own_columns(branch, (t + k) % parts)
            total = total + shift(theirs, "tp", parts, k).astype(jnp.float32)
        return (own_columns(residual, t) + 0.5 * total).astype(jnp.bfloat16)

    return shards


def solution(mesh):
    in_specs = (
        P(("grp", "fs"), "tp"),
        P(),
        P("fs", "tp"),
        P("fs", "tp"),
        P("tp", "fs"),
        P(),
        P("fs", "tp"),
        P("fs", "tp"),
        P("fs", "tp"),
        P(None, "tp"),
        P("tp", "fs"),
        P(),
        P("fs", "tp"),
        P("fs", "tp"),
        P("tp", "fs"),
    )
    out_specs = P(("grp", "fs"), "tp")
    shards = make_shards(mesh.shape["grp"], mesh.shape["fs"], mesh.shape["tp"])
    return jax.shard_map(shards, mesh=mesh, in_specs=in_specs, out_specs=out_specs, check_vma=False)
```
